32 devices in a mesh: sp: 16 (over z, y, x), tp: 2 (over core).
Axes of the slice: x: 2, y: 2, z: 4, core: 2. Of those that a mesh axis runs over, the one named last changes fastest.
Arguments:
- tokens: bfloat16 [4096, 2048], P('sp'), as said below
- in_gain: float32 [2048], replicated, may hold values from 0.1 to 1.9
- w_query: bfloat16 [2048, 1024], P(None, 'tp'), as said below
- w_key: bfloat16 [2048, 1024], P(None, 'tp'), may hold values from -0.125 to 0.125
- w_value: bfloat16 [2048, 1024], P(None, 'tp'), may hold values from -0.125 to 0.125
- lam: float32 [8], P('tp'), may hold values from 0.3 to 0.8
- sub_gain: float32 [128], replicated, may hold values from 0.1 to 1.9
- w_out: bfloat16 [1024, 2048], P('tp'), may hold values from -0.1875 to 0.1875
Outputs:
- mixed: bfloat16 [4096, 2048], P('sp')
The draws below stay inside these ranges and needn't reach their ends.
Inputs may be any that keep to these rules, and one draw needn't show every extreme that they name: tokens: normal entries plus, for each block of 64 tokens, a factor times one direction common to all tokens. w_query: independent normal entries.
All inputs are finite; a program needn't handle non-finite values.
Results may differ from the reference program's by a relative error of at most 0.025.
The reference program's roundings to bfloat16 on the way (of `normed`, `values`, `weights` and `attended`) count: a program that leaves them out, or rounds other values in their place, can miss the bound.
Values may be sent and summed in bfloat16 or wider, within the bound.
A program may use at most 64 MiB of HBM per device.

```python
import jax
import jax.numpy as jnp
from jax import lax

D = 2048
HEADS = 8
KD = 64
VD = 128
TOKENS = 4096


def draw_tokens(key, part):
    first, second, third = jax.random.split(jax.random.fold_in(key, 11), 3)
    base = jax.random.normal(first, (TOKENS, D), jnp.float32)
    direction = jax.random.normal(second, (D,), jnp.float32)
    factor = jax.random.uniform(third, (TOKENS // 64,), jnp.float32, -1.5, 1.5)
    whole = base + jnp.repeat(factor, 64)[:, None] * direction[None, :]
    return jnp.clip(whole, -12.0, 12.0).astype(jnp.bfloat16)


def draw_w_query(key, part):
    base = jnp.clip(jax.random.normal(jax.random.fold_in(key, 23), (D, HEADS * 2 * KD), jnp.float32), -6.0, 6.0)
    scaled = base * (1.7 / jnp.sqrt(jnp.float32(D)))
    return scaled.astype(jnp.bfloat16)


def shard_levels(own_key, shape, shards, smallest, largest):
    gain = 1.0
    for axis_at, shards_of in shards:
        draws = jax.random.uniform(jax.random.fold_in(jax.random.fold_in(own_key, 6), axis_at), (shards_of,), jnp.float32, smallest / len(shards), largest / len(shards))
        gain = gain * jnp.repeat(jnp.exp(draws), shape[axis_at] // shards_of).reshape((-1,) + (1,) * (len(shape) - 1 - axis_at))
    return gain


def noise(key, shape, deviation, limit, cuts=(), held_as=jnp.bfloat16):
    drawn = deviation * jax.random.normal(key, shape, jnp.float32)
    if cuts:
        drawn = drawn * shard_levels(key, shape, cuts, -0.22, 0.18)
    return jnp.clip(drawn, -limit, limit).astype(held_as)


def setup_inputs(seed: int = 0) -> dict:
    streams_of = jax.random.split(jax.random.key(seed), 9)
    return {
        "tokens": draw_tokens(jax.random.fold_in(streams_of[8], 71), 0),
        "in_gain": jnp.clip(1.0 + 0.18 * jax.random.normal(streams_of[1], (D,), jnp.float32), 0.1, 1.9),
        "w_query": draw_w_query(jax.random.fold_in(streams_of[8], 71), 0),
        "w_key": noise(streams_of[3], (D, HEADS * 2 * KD), D ** -0.5, 0.125, ((1, 2),)),
        "w_value": noise(streams_of[4], (D, HEADS * VD), D ** -0.5, 0.125, ((1, 2),)),
        "lam": jnp.clip(0.3 + 0.5 * jax.random.uniform(streams_of[5], (HEADS,), jnp.float32) ** shard_levels(streams_of[5], (HEADS,), ((0, 2),), -0.2, 0.2), 0.3, 0.8),
        "sub_gain": jnp.clip(1.0 + 0.18 * jax.random.normal(streams_of[6], (VD,), jnp.float32), 0.1, 1.9),
        "w_out": noise(streams_of[7], (HEADS * VD, D), (HEADS * VD) ** -0.5, 0.1875, ((0, 2),)),
    }


def rotate(vectors, position):
    half = vectors.shape[-1] // 2
    freq = 500000.0 ** (-jnp.arange(0, 2 * half, 2, dtype=jnp.float32) / (2 * half))
    angle = position.astype(jnp.float32)[:, None] * freq[None, :]
    cosine = jnp.cos(angle)[:, None, :]
    sine = jnp.sin(angle)[:, None, :]
    first = vectors[..., :half]
    second = vectors[..., half:]
    return jnp.concatenate([first * cosine - second * sine, second * cosine + first * sine], axis=-1)

def reference(tokens, in_gain, w_query, w_key, w_value, lam, sub_gain, w_out):
    total = tokens.shape[0]
    xfloat = tokens.astype(jnp.float32)
    normed = (xfloat * lax.rsqrt(lax.optimization_barrier(jnp.mean(xfloat * xfloat, axis=-1, keepdims=True)) + 1e-06) * in_gain).astype(jnp.bfloat16)
    position = jnp.arange(total, dtype=jnp.int32)
    queries = rotate(jnp.dot(normed, w_query, preferred_element_type=jnp.float32).reshape(total, 2 * HEADS, KD), position).astype(jnp.bfloat16)
    keys = rotate(jnp.dot(normed, w_key, preferred_element_type=jnp.float32).reshape(total, 2 * HEADS, KD), position).astype(jnp.bfloat16)
    values = jnp.dot(normed, w_value, preferred_element_type=jnp.float32).astype(jnp.bfloat16).reshape(total, HEADS, VD)
    queries = jnp.transpose(queries.reshape(total, HEADS, 2, KD), (1, 0, 2, 3))
    keys = jnp.transpose(keys.reshape(total, HEADS, 2, KD), (1, 0, 2, 3))
    values = jnp.transpose(values, (1, 0, 2))
    block = min(512, total)
    scale = KD ** (-0.5)

    def one_head(items):
        query_h, key_h, value_h, lam_h = items
        keyf = key_h.astype(jnp.float32)
        valuef = value_h.astype(jnp.float32)

        def one_block(query_b):
            scores = jnp.einsum('qcd,kcd->cqk', query_b.astype(jnp.float32), keyf) * scale
            top = lax.optimization_barrier(jnp.max(scores, axis=-1, keepdims=True))
            expo = jnp.exp(scores - top)
            mass = lax.optimization_barrier(jnp.sum(expo, axis=-1))
            weights = expo.astype(jnp.bfloat16).astype(jnp.float32)
            read = jnp.einsum('cqk,ke->cqe', weights, valuef) / mass[..., None]
            diff = read[0] - lam_h * read[1]
            normal = diff * lax.rsqrt(lax.optimization_barrier(jnp.mean(diff * diff, axis=-1, keepdims=True)) + 1e-05) * sub_gain
            return normal.astype(jnp.bfloat16)
        blocks = query_h.reshape(total // block, block, 2, KD)
        return lax.map(one_block, blocks).reshape(total, VD)
    heads = lax.map(one_head, (queries, keys, values, lam))
    attended = jnp.transpose(heads, (1, 0, 2)).reshape(total, HEADS * VD)
    return jnp.dot(attended, w_out, preferred_element_type=jnp.float32).astype(jnp.bfloat16)
```

```python
import functools

import jax
import jax.numpy as jnp
from jax import lax
from jax.experimental import pallas as pl
from jax.experimental.pallas import tpu as pltpu
from jax.sharding import PartitionSpec as P

KD = 64
VD = 128
HW = 2 * KD
MESH = pl.DeviceIdType.MESH
LOG2E = 1.4426950408889634


def kernel(
    dims,
    tok_hbm,
    gain_ref,
    wq_hbm,
    wk_hbm,
    wv_hbm,
    lam_ref,
    sub_ref,
    wo_hbm,
    cos_ref,
    sin_ref,
    out_ref,
    tok,
    wq,
    wk,
    wv,
    wo,
    normed,
    qst,
    kst,
    vst,
    qbuf,
    kbuf,
    vbuf,
    acc,
    top,
    mass,
    attst,
    att,
    load_sem,
    send_sem,
    q_sem,
    k_sem,
    v_sem,
    a_sem,
    w_sem,
):
    H, R, TP, span = dims
    sp = lax.axis_index("sp")
    tpi = lax.axis_index("tp")
    g = sp // R
    r = sp % R
    sent = []

    def head_peer(d):
        return (g + d) % H

    def row_peer(d):
        if R == 4:
            x, y = r % 2, r // 2
            return [None, y * 2 + (1 - x), (1 - y) * 2 + x, 3 - r][d]
        return (r + d) % R

    def at(group, row):
        return {"sp": group * R + row}

    def remote(src, dst, recv, device):
        copy = pltpu.make_async_remote_copy(
            src_ref=src,
            dst_ref=dst,
            send_sem=send_sem.at[len(sent)],
            recv_sem=recv,
            device_id=device,
            device_id_type=MESH,
        )
        copy.start()
        sent.append(copy)

    def arrived(dst, recv):
        pltpu.make_async_remote_copy(
            src_ref=dst,
            dst_ref=dst,
            send_sem=send_sem.at[0],
            recv_sem=recv,
            device_id={"tp": (tpi + 1) % TP},
            device_id_type=MESH,
        ).wait_recv()

    loads = [
        pltpu.make_async_copy(tok_hbm, tok, load_sem.at[0]),
        pltpu.make_async_copy(wq_hbm, wq, load_sem.at[1]),
        pltpu.make_async_copy(wk_hbm, wk, load_sem.at[2]),
        pltpu.make_async_copy(wv_hbm, wv, load_sem.at[3]),
        pltpu.make_async_copy(
            wo_hbm, wo.at[pl.ds(pl.multiple_of(tpi * (H * VD), VD), H * VD)], load_sem.at[4]
        ),
    ]
    for load in loads[:4]:
        load.start()

    barrier = pltpu.get_barrier_semaphore()
    for d in range(1, H):
        pl.semaphore_signal(barrier, inc=1, device_id=at(head_peer(d), r), device_id_type=MESH)
    for d in range(1, R):
        pl.semaphore_signal(barrier, inc=1, device_id=at(g, row_peer(d)), device_id_type=MESH)
    for d in range(1, TP):
        pl.semaphore_signal(barrier, inc=1, device_id={"tp": (tpi + d) % TP}, device_id_type=MESH)

    loads[0].wait()
    rows = 32

    def norm_rows(i, carry):
        part = pl.ds(pl.multiple_of(i * rows, rows), rows)
        x = tok[part, :].astype(jnp.float32)
        mean = jnp.mean(x * x, axis=-1, keepdims=True)
        normed[part, :] = (x * lax.rsqrt(mean + 1e-06) * gain_ref[...]).astype(jnp.bfloat16)
        return carry

    lax.fori_loop(0, span // rows, norm_rows, 0)

    lane = lax.broadcasted_iota(jnp.int32, (span, HW), 1)
    low = (lane % KD) < (KD // 2)

    def rotated(x):
        other = jnp.where(low, pltpu.roll(x, HW - KD // 2, 1), pltpu.roll(x, KD // 2, 1))
        return (x * cos_ref[...] + other * sin_ref[...]).astype(jnp.bfloat16)

    def project(weight, stage, turn):
        y = jnp.dot(normed[...], weight[...], preferred_element_type=jnp.float32)
        for h in range(H):
            z = y[:, h * HW : (h + 1) * HW]
            stage[h] = rotated(z) if turn else z.astype(jnp.bfloat16)

    loads[1].wait()
    project(wq, qst, True)
    pl.semaphore_wait(barrier, (H - 1) + (R - 1) + (TP - 1))
    for d in range(1, H):
        to = head_peer(d)
        remote(qst.at[to], qbuf.at[g], q_sem.at[g], at(to, r))
    qbuf[g] = qst[g]
    for weight, stage, buf, sem, load in (
        (wk, kst, kbuf, k_sem, loads[2]),
        (wv, vst, vbuf, v_sem, loads[3]),
    ):
        load.wait()
        project(weight, stage, stage is kst)
        for d in range(1, H):
            to = head_peer(d)
            remote(stage.at[to], buf.at[g, r], sem.at[g, r], at(to, r))
        buf[g, r] = stage[g]
        for d in range(1, R):
            remote(stage.at[g], buf.at[g, r], sem.at[g, r], at(g, row_peer(d)))
    own_rows = pl.ds(pl.multiple_of(tpi * (H * VD), VD), H * VD)
    loads[4].start()
    for d in range(1, TP):
        remote(wo_hbm, wo.at[own_rows], w_sem.at[tpi], {"tp": (tpi + d) % TP})

    def spread(s):
        gs = head_peer(s)
        for buf, sem in ((kbuf, k_sem), (vbuf, v_sem)):
            arrived(buf.at[gs, r], sem.at[gs, r])
            for d in range(1, R):
                remote(buf.at[gs, r], buf.at[gs, r], sem.at[gs, r], at(g, row_peer(d)))

    RC = max(1, min(R, 1024 // span))
    while R % RC:
        RC -= 1
    nu = R // RC
    keys = RC * span
    scale = LOG2E * KD ** (-0.5)

    def attend(gs, u, t, first):
        kb = kbuf[gs, pl.ds(u * RC, RC)].reshape(keys, HW)
        vb = vbuf[gs, pl.ds(u * RC, RC)].reshape(keys, VD)
        q = qbuf[t]
        for c in range(2):
            qc = jnp.where((lane // KD) == c, q, jnp.zeros_like(q))
            s = lax.dot_general(
                qc, kb, (((1,), (1,)), ((), ())), preferred_element_type=jnp.float32
            )
            new = jnp.max(s, axis=-1, keepdims=True) * scale
            if not first:
                old = top[t, c][:, :1]
                new = jnp.maximum(new, old)
            p = jnp.exp2(s * scale - new)
            total = jnp.sum(p, axis=-1, keepdims=True)
            read = jnp.dot(p.astype(jnp.bfloat16), vb, preferred_element_type=jnp.float32)
            if first:
                acc[t, c] = read
                mass[t, c] = jnp.broadcast_to(total, (span, VD))
            else:
                factor = jnp.exp2(old - new)
                acc[t, c] = acc[t, c] * factor + read
                mass[t, c] = mass[t, c] * factor + total
            top[t, c] = jnp.broadcast_to(new, (span, VD))

    def finish(t):
        diff = acc[t, 0] / mass[t, 0] - lam_ref[g] * (acc[t, 1] / mass[t, 1])
        mean = jnp.mean(diff * diff, axis=-1, keepdims=True)
        return (diff * lax.rsqrt(mean + 1e-05) * sub_ref[...]).astype(jnp.bfloat16)

    def column(tp, h):
        return pl.ds(pl.multiple_of((tp * H + h) * VD, VD), VD)

    for d in range(1, H):
        arrived(qbuf.at[head_peer(d)], q_sem.at[head_peer(d)])

    if nu > 1:
        top[...] = jnp.full(top.shape, -1e30, jnp.float32)
        mass[...] = jnp.zeros(mass.shape, jnp.float32)
        acc[...] = jnp.zeros(acc.shape, jnp.float32)

    def finish_and_send(j):
        t = (g + 1 + j) % H
        done = finish(t)
        if j == H - 1:
            att[:, column(tpi, g)] = done
        else:
            attst[j] = done
            remote(attst.at[j], att.at[:, column(tpi, g)], a_sem.at[tpi * H + g], at(t, r))

    for s in range(H):
        gs = head_peer(s)
        if s + 1 < H:
            spread(s + 1)
        for d in range(1, R):
            rs = row_peer(d)
            arrived(kbuf.at[gs, rs], k_sem.at[gs, rs])
            arrived(vbuf.at[gs, rs], v_sem.at[gs, rs])
        if nu > 1:

            def chunk(i, carry):
                attend(gs, i // H, i % H, False)
                return carry

            lax.fori_loop(0, nu * H, chunk, 0)
        elif s < H - 1:

            def tile(t, carry):
                attend(gs, 0, t, s == 0)
                return carry

            lax.fori_loop(0, H, tile, 0)
        else:
            for j in range(H):
                attend(gs, 0, (g + 1 + j) % H, s == 0)
                finish_and_send(j)
    if nu > 1:
        for j in range(H):
            finish_and_send(j)

    def pass_on(h):
        for d in range(1, TP):
            remote(
                att.at[:, column(tpi, h)],
                att.at[:, column(tpi, h)],
                a_sem.at[tpi * H + h],
                {"tp": (tpi + d) % TP},
            )

    pass_on(g)
    for d in range(H - 1, 0, -1):
        h = head_peer(d)
        arrived(att.at[:, column(tpi, h)], a_sem.at[tpi * H + h])
        pass_on(h)
    loads[4].wait()
    for d in range(1, TP):
        other = (tpi + d) % TP
        arrived(wo.at[pl.ds(pl.multiple_of(other * (H * VD), VD), H * VD)], w_sem.at[other])
        for h in range(H):
            arrived(att.at[:, column(other, h)], a_sem.at[other * H + h])

    width = min(512, out_ref.shape[1])
    for n in range(out_ref.shape[1] // width):
        part = slice(n * width, (n + 1) * width)
        out_ref[:, part] = jnp.dot(
            att[...], wo[:, part], preferred_element_type=jnp.float32
        ).astype(out_ref.dtype)
    for copy in sent:
        copy.wait_send()


def shards(sp_size, tp_size, tokens, in_gain, w_query, w_key, w_value, lam, sub_gain, w_out):
    span, model = tokens.shape
    H = lam.shape[0]
    R = sp_size // H
    TP = tp_size
    half = KD // 2
    freq = 500000.0 ** (-jnp.arange(0, 2 * half, 2, dtype=jnp.float32) / (2 * half))
    position = lax.axis_index("sp") * span + jnp.arange(span, dtype=jnp.int32)
    angle = position.astype(jnp.float32)[:, None] * freq[None, :]
    cosine = jnp.cos(angle)
    sine = jnp.sin(angle)
    cosine = jnp.concatenate([cosine] * 4, axis=1)
    sine = jnp.concatenate([-sine, sine] * 2, axis=1)
    bf16, f32 = jnp.bfloat16, jnp.float32
    sends = 3 * (H - 1) + 2 * H * (R - 1) + (TP - 1) + (H - 1) + H * (TP - 1)
    hbm = pl.BlockSpec(memory_space=pl.ANY)
    vmem = pl.BlockSpec(memory_space=pltpu.VMEM)
    smem = pl.BlockSpec(memory_space=pltpu.SMEM)
    DMA = pltpu.SemaphoreType.DMA
    return pl.pallas_call(
        functools.partial(kernel, (H, R, TP, span)),
        out_shape=jax.ShapeDtypeStruct((span, model), bf16),
        in_specs=[hbm, vmem, hbm, hbm, hbm, smem, vmem, hbm, vmem, vmem],
        out_specs=vmem,
        scratch_shapes=[
            pltpu.VMEM(tokens.shape, bf16),
            pltpu.VMEM(w_query.shape, bf16),
            pltpu.VMEM(w_key.shape, bf16),
            pltpu.VMEM(w_value.shape, bf16),
            pltpu.VMEM((TP * H * VD, model), bf16),
            pltpu.VMEM(tokens.shape, bf16),
            pltpu.VMEM((H, span, HW), bf16),
            pltpu.VMEM((H, span, HW), bf16),
            pltpu.VMEM((H, span, VD), bf16),
            pltpu.VMEM((H, span, HW), bf16),
            pltpu.VMEM((H, R, span, HW), bf16),
            pltpu.VMEM((H, R, span, VD), bf16),
            pltpu.VMEM((H, 2, span, VD), f32),
            pltpu.VMEM((H, 2, span, VD), f32),
            pltpu.VMEM((H, 2, span, VD), f32),
            pltpu.VMEM((max(1, H - 1), span, VD), bf16),
            pltpu.VMEM((span, TP * H * VD), bf16),
            DMA((5,)),
            DMA((sends,)),
            DMA((H,)),
            DMA((H, R)),
            DMA((H, R)),
            DMA((TP * H,)),
            DMA((TP,)),
        ],
        compiler_params=pltpu.CompilerParams(
            collective_id=0, has_side_effects=True, vmem_limit_bytes=60 * 1024 * 1024
        ),
        name="layer",
    )(
        tokens,
        in_gain.reshape(1, -1),
        w_query,
        w_key,
        w_value,
        lam,
        sub_gain.reshape(1, -1),
        w_out,
        cosine,
        sine,
    )


def solution(mesh):
    in_specs = (
        P("sp", None),
        P(),
        P(None, "tp"),
        P(None, "tp"),
        P(None, "tp"),
        P("tp"),
        P(),
        P("tp", None),
    )
    out_specs = P("sp", None)
    body = functools.partial(shards, mesh.shape["sp"], mesh.shape["tp"])
    return jax.shard_map(body, mesh=mesh, in_specs=in_specs, out_specs=out_specs, check_vma=False)
```

```python
import functools

import jax
import jax.numpy as jnp
from jax import lax
from jax.experimental import pallas as pl
from jax.experimental.pallas import tpu as pltpu
from jax.sharding import PartitionSpec as P

KD = 64
VD = 128
HW = 2 * KD
MESH = pl.DeviceIdType.MESH
LOG2E = 1.4426950408889634


def kernel(
    dims,
    tok_hbm,
    gain_ref,
    wq_hbm,
    wk_hbm,
    wv_hbm,
    lam_ref,
    sub_ref,
    wo_hbm,
    cos_ref,
    sin_ref,
    out_ref,
    tok,
    wq,
    wk,
    wv,
    wo,
    normed,
    qst,
    kst,
    vst,
    qbuf,
    kbuf,
    vbuf,
    acc,
    top,
    mass,
    attst,
    att,
    load_sem,
    send_sem,
    q_sem,
    k_sem,
    v_sem,
    a_sem,
    w_sem,
):
    H, R, TP, span = dims
    sp = lax.axis_index("sp")
    tpi = lax.axis_index("tp")
    g = sp // R
    r = sp % R
    sent = []

    def head_peer(d):
        return (g + d) % H

    def row_peer(d):
        if R == 4:
            x, y = r % 2, r // 2
            return [None, y * 2 + (1 - x), (1 - y) * 2 + x, 3 - r][d]
        return (r + d) % R

    def at(group, row):
        return {"sp": group * R + row}

    def remote(src, dst, recv, device):
        copy = pltpu.make_async_remote_copy(
            src_ref=src,
            dst_ref=dst,
            send_sem=send_sem.at[len(sent)],
            recv_sem=recv,
            device_id=device,
            device_id_type=MESH,
        )
        copy.start()
        sent.append(copy)

    def arrived(dst, recv):
        pltpu.make_async_remote_copy(
            src_ref=dst,
            dst_ref=dst,
            send_sem=send_sem.at[0],
            recv_sem=recv,
            device_id={"tp": (tpi + 1) % TP},
            device_id_type=MESH,
        ).wait_recv()

    loads = [
        pltpu.make_async_copy(tok_hbm, tok, load_sem.at[0]),
        pltpu.make_async_copy(wq_hbm, wq, load_sem.at[1]),
        pltpu.make_async_copy(wk_hbm, wk, load_sem.at[2]),
        pltpu.make_async_copy(wv_hbm, wv, load_sem.at[3]),
        pltpu.make_async_copy(
            wo_hbm, wo.at[pl.ds(pl.multiple_of(tpi * (H * VD), VD), H * VD)], load_sem.at[4]
        ),
    ]
    for load in loads[:4]:
        load.start()

    barrier = pltpu.get_barrier_semaphore()
    for d in range(1, H):
        pl.semaphore_signal(barrier, inc=1, device_id=at(head_peer(d), r), device_id_type=MESH)
    for d in range(1, R):
        pl.semaphore_signal(barrier, inc=1, device_id=at(g, row_peer(d)), device_id_type=MESH)
    for d in range(1, TP):
        pl.semaphore_signal(barrier, inc=1, device_id={"tp": (tpi + d) % TP}, device_id_type=MESH)

    loads[0].wait()
    rows = 32

    def norm_rows(i, carry):
        part = pl.ds(pl.multiple_of(i * rows, rows), rows)
        x = tok[part, :].astype(jnp.float32)
        mean = jnp.mean(x * x, axis=-1, keepdims=True)
        normed[part, :] = (x * lax.rsqrt(mean + 1e-06) * gain_ref[...]).astype(jnp.bfloat16)
        return carry

    lax.fori_loop(0, span // rows, norm_rows, 0)

    lane = lax.broadcasted_iota(jnp.int32, (span, HW), 1)
    low = (lane % KD) < (KD // 2)

    def rotated(x):
        other = jnp.where(low, pltpu.roll(x, HW - KD // 2, 1), pltpu.roll(x, KD // 2, 1))
        return (x * cos_ref[...] + other * sin_ref[...]).astype(jnp.bfloat16)

    def project(weight, stage, turn):
        y = jnp.dot(normed[...], weight[...], preferred_element_type=jnp.float32)
        for h in range(H):
            z = y[:, h * HW : (h + 1) * HW]
            stage[h] = rotated(z) if turn else z.astype(jnp.bfloat16)

    loads[1].wait()
    project(wq, qst, True)
    pl.semaphore_wait(barrier, (H - 1) + (R - 1) + (TP - 1))
    for d in range(1, H):
        to = head_peer(d)
        remote(qst.at[to], qbuf.at[g], q_sem.at[g], at(to, r))
    qbuf[g] = qst[g]
    for weight, stage, buf, sem, load in (
        (wk, kst, kbuf, k_sem, loads[2]),
        (wv, vst, vbuf, v_sem, loads[3]),
    ):
        load.wait()
        project(weight, stage, stage is kst)
        for d in range(H - 1, 0, -1):
            to = head_peer(d)
            remote(stage.at[to], buf.at[g, r], sem.at[g, r], at(to, r))
        buf[g, r] = stage[g]
        for d in range(1, R):
            remote(stage.at[g], buf.at[g, r], sem.at[g, r], at(g, row_peer(d)))
    own_rows = pl.ds(pl.multiple_of(tpi * (H * VD), VD), H * VD)
    loads[4].start()
    for d in range(1, TP):
        remote(wo_hbm, wo.at[own_rows], w_sem.at[tpi], {"tp": (tpi + d) % TP})

    def spread(s):
        gs = head_peer(s)
        for buf, sem in ((kbuf, k_sem), (vbuf, v_sem)):
            arrived(buf.at[gs, r], sem.at[gs, r])
            for d in range(1, R):
                remote(buf.at[gs, r], buf.at[gs, r], sem.at[gs, r], at(g, row_peer(d)))

    RC = max(1, min(R, 1024 // span))
    while R % RC:
        RC -= 1
    nu = R // RC
    keys = RC * span
    scale = LOG2E * KD ** (-0.5)

    def attend(gs, u, t, first):
        kb = kbuf[gs, pl.ds(u * RC, RC)].reshape(keys, HW)
        vb = vbuf[gs, pl.ds(u * RC, RC)].reshape(keys, VD)
        q = qbuf[t]
        for c in range(2):
            qc = jnp.where((lane // KD) == c, q, jnp.zeros_like(q))
            s = lax.dot_general(
                qc, kb, (((1,), (1,)), ((), ())), preferred_element_type=jnp.float32
            )
            new = jnp.max(s, axis=-1, keepdims=True) * scale
            if not first:
                old = top[t, c][:, :1]
                new = jnp.maximum(new, old)
            p = jnp.exp2(s * scale - new)
            total = jnp.sum(p, axis=-1, keepdims=True)
            read = jnp.dot(p.astype(jnp.bfloat16), vb, preferred_element_type=jnp.float32)
            if first:
                acc[t, c] = read
                mass[t, c] = jnp.broadcast_to(total, (span, VD))
            else:
                factor = jnp.exp2(old - new)
                acc[t, c] = acc[t, c] * factor + read
                mass[t, c] = mass[t, c] * factor + total
            top[t, c] = jnp.broadcast_to(new, (span, VD))

    def finish(t):
        diff = acc[t, 0] / mass[t, 0] - lam_ref[g] * (acc[t, 1] / mass[t, 1])
        mean = jnp.mean(diff * diff, axis=-1, keepdims=True)
        return (diff * lax.rsqrt(mean + 1e-05) * sub_ref[...]).astype(jnp.bfloat16)

    def column(tp, h):
        return pl.ds(pl.multiple_of((tp * H + h) * VD, VD), VD)

    for d in range(1, H):
        arrived(qbuf.at[head_peer(d)], q_sem.at[head_peer(d)])

    if nu > 1:
        top[...] = jnp.full(top.shape, -1e30, jnp.float32)
        mass[...] = jnp.zeros(mass.shape, jnp.float32)
        acc[...] = jnp.zeros(acc.shape, jnp.float32)

    def finish_and_send(j):
        t = (g + 1 + j) % H
        done = finish(t)
        if j == H - 1:
            att[:, column(tpi, g)] = done
        else:
            attst[j] = done
            remote(attst.at[j], att.at[:, column(tpi, g)], a_sem.at[tpi * H + g], at(t, r))

    for s in range(H):
        gs = head_peer(s)
        if s + 1 < H:
            spread(s + 1)
        for d in range(1, R):
            rs = row_peer(d)
            arrived(kbuf.at[gs, rs], k_sem.at[gs, rs])
            arrived(vbuf.at[gs, rs], v_sem.at[gs, rs])
        if nu > 1:

            def chunk(i, carry):
                attend(gs, i // H, i % H, False)
                return carry

            lax.fori_loop(0, nu * H, chunk, 0)
        elif s < H - 1:

            def tile(t, carry):
                attend(gs, 0, t, s == 0)
                return carry

            lax.fori_loop(0, H, tile, 0)
        else:
            for j in range(H):
                attend(gs, 0, (g + 1 + j) % H, s == 0)
                finish_and_send(j)
    if nu > 1:
        for j in range(H):
            finish_and_send(j)

    def pass_on(h):
        for d in range(1, TP):
            remote(
                att.at[:, column(tpi, h)],
                att.at[:, column(tpi, h)],
                a_sem.at[tpi * H + h],
                {"tp": (tpi + d) % TP},
            )

    pass_on(g)
    for d in range(H - 1, 0, -1):
        h = head_peer(d)
        arrived(att.at[:, column(tpi, h)], a_sem.at[tpi * H + h])
        pass_on(h)
    loads[4].wait()
    for d in range(1, TP):
        other = (tpi + d) % TP
        arrived(wo.at[pl.ds(pl.multiple_of(other * (H * VD), VD), H * VD)], w_sem.at[other])
        for h in range(H):
            arrived(att.at[:, column(other, h)], a_sem.at[other * H + h])

    width = min(512, out_ref.shape[1])
    for n in range(out_ref.shape[1] // width):
        part = slice(n * width, (n + 1) * width)
        out_ref[:, part] = jnp.dot(
            att[...], wo[:, part], preferred_element_type=jnp.float32
        ).astype(out_ref.dtype)
    for copy in sent:
        copy.wait_send()


def shards(sp_size, tp_size, tokens, in_gain, w_query, w_key, w_value, lam, sub_gain, w_out):
    span, model = tokens.shape
    H = lam.shape[0]
    R = sp_size // H
    TP = tp_size
    half = KD // 2
    freq = 500000.0 ** (-jnp.arange(0, 2 * half, 2, dtype=jnp.float32) / (2 * half))
    position = lax.axis_index("sp") * span + jnp.arange(span, dtype=jnp.int32)
    angle = position.astype(jnp.float32)[:, None] * freq[None, :]
    cosine = jnp.cos(angle)
    sine = jnp.sin(angle)
    cosine = jnp.concatenate([cosine] * 4, axis=1)
    sine = jnp.concatenate([-sine, sine] * 2, axis=1)
    bf16, f32 = jnp.bfloat16, jnp.float32
    sends = 3 * (H - 1) + 2 * H * (R - 1) + (TP - 1) + (H - 1) + H * (TP - 1)
    hbm = pl.BlockSpec(memory_space=pl.ANY)
    vmem = pl.BlockSpec(memory_space=pltpu.VMEM)
    smem = pl.BlockSpec(memory_space=pltpu.SMEM)
    DMA = pltpu.SemaphoreType.DMA
    return pl.pallas_call(
        functools.partial(kernel, (H, R, TP, span)),
        out_shape=jax.ShapeDtypeStruct((span, model), bf16),
        in_specs=[hbm, vmem, hbm, hbm, hbm, smem, vmem, hbm, vmem, vmem],
        out_specs=vmem,
        scratch_shapes=[
            pltpu.VMEM(tokens.shape, bf16),
            pltpu.VMEM(w_query.shape, bf16),
            pltpu.VMEM(w_key.shape, bf16),
            pltpu.VMEM(w_value.shape, bf16),
            pltpu.VMEM((TP * H * VD, model), bf16),
            pltpu.VMEM(tokens.shape, bf16),
            pltpu.VMEM((H, span, HW), bf16),
            pltpu.VMEM((H, span, HW), bf16),
            pltpu.VMEM((H, span, VD), bf16),
            pltpu.VMEM((H, span, HW), bf16),
            pltpu.VMEM((H, R, span, HW), bf16),
            pltpu.VMEM((H, R, span, VD), bf16),
            pltpu.VMEM((H, 2, span, VD), f32),
            pltpu.VMEM((H, 2, span, VD), f32),
            pltpu.VMEM((H, 2, span, VD), f32),
            pltpu.VMEM((max(1, H - 1), span, VD), bf16),
            pltpu.VMEM((span, TP * H * VD), bf16),
            DMA((5,)),
            DMA((sends,)),
            DMA((H,)),
            DMA((H, R)),
            DMA((H, R)),
            DMA((TP * H,)),
            DMA((TP,)),
        ],
        compiler_params=pltpu.CompilerParams(
            collective_id=0, has_side_effects=True, vmem_limit_bytes=60 * 1024 * 1024
        ),
        name="layer",
    )(
        tokens,
        in_gain.reshape(1, -1),
        w_query,
        w_key,
        w_value,
        lam,
        sub_gain.reshape(1, -1),
        w_out,
        cosine,
        sine,
    )


def solution(mesh):
    in_specs = (
        P("sp", None),
        P(),
        P(None, "tp"),
        P(None, "tp"),
        P(None, "tp"),
        P("tp"),
        P(),
        P("tp", None),
    )
    out_specs = P("sp", None)
    body = functools.partial(shards, mesh.shape["sp"], mesh.shape["tp"])
    return jax.shard_map(body, mesh=mesh, in_specs=in_specs, out_specs=out_specs, check_vma=False)
```
